32 devices in a mesh: sp: 8 (over z, x), tp: 4 (over y, core).
Axes of the slice: x: 2, y: 2, z: 4, core: 2. Of those that a mesh axis runs over, the one named last changes fastest.
Arguments:
- tokens_in: bfloat16 [4096, 4096], P(('sp', 'tp')), may hold values from -64 to 64
- w_query: bfloat16 [4096, 2048], P(None, 'tp'), may hold values from -0.09375 to 0.09375
- w_key: bfloat16 [4096, 2048], P(None, 'tp'), may hold values from -0.09375 to 0.09375
- w_value: bfloat16 [4096, 2048], P(None, 'tp'), may hold values from -0.09375 to 0.09375
- w_out: bfloat16 [2048, 4096], P('tp'), may hold values from -1 to 1
Outputs:
- mixed: bfloat16 [4096, 4096], P(('sp', 'tp'))
- log_weight: float32 [32, 4096], P('tp', 'sp')
The draws below stay inside these ranges and needn't reach their ends.
All inputs are finite; a program needn't handle non-finite values.
Results may differ from the reference program's by a relative error of at most 0.019.
Values may be sent and summed in bfloat16 or wider, within the bound.
A program may use at most 128 MiB of HBM per device.

```python
import jax
import jax.numpy as jnp
from jax import lax

D = 4096
HEADS = 32
HEAD_DIM = 64
SIDE_SPAN = 64
MIDDLE_DILATION = 8
WIDEST_DILATION = 64
TOKENS = 4096
N_TP = 4


def draw_tokens_in(key, part):
    base_key = jax.random.fold_in(jax.random.fold_in(key, 11), 0)
    values = jax.random.truncated_normal(base_key, -4.0, 4.0, (TOKENS, D), jnp.float32)
    return values.astype(jnp.bfloat16)


def steps_of(own_key, extent, cuts, low, high):
    def one(dim, shards_of):
        draws = jax.random.uniform(jax.random.fold_in(jax.random.fold_in(own_key, 6), dim), (shards_of,), jnp.float32, low / len(cuts), high / len(cuts))
        return jnp.repeat(jnp.exp(draws), extent[dim] // shards_of).reshape((-1,) + (1,) * (len(extent) - dim - 1))

    gain = one(*cuts[0])
    for cut in cuts[1:]:
        gain = gain * one(*cut)
    return gain


def gaussian(key, dims, scale, bound, shards=(), kind=jnp.bfloat16):
    entries = scale * jax.random.normal(key, dims, jnp.float32)
    if shards:
        entries = entries * steps_of(key, dims, shards, -0.22, 0.18)
    return jnp.clip(entries, -bound, bound).astype(kind)


def setup_inputs(seed: int = 0) -> dict:
    arg_keys = jax.random.split(jax.random.key(seed), 6)
    tokens_in = draw_tokens_in(jax.random.fold_in(arg_keys[5], 71), 0)
    w_query = gaussian(arg_keys[1], (D, HEADS * HEAD_DIM), D ** -0.5, 0.09375, ((1, 4),))
    w_key = gaussian(arg_keys[2], (D, HEADS * HEAD_DIM), D ** -0.5, 0.09375, ((1, 4),))
    w_value = gaussian(arg_keys[3], (D, HEADS * HEAD_DIM), D ** -0.5, 0.09375, ((1, 4),))
    w_out = gaussian(arg_keys[4], (HEADS * HEAD_DIM, D), HEADS ** -0.5, 1.0, ((0, 4),))
    return {"tokens_in": tokens_in, "w_query": w_query, "w_key": w_key, "w_value": w_value, "w_out": w_out}


ROTARY_BASE = 500000.0
NEGATIVE = -1e30


def rotate(block, positions):
    half_size = block.shape[-1] // 2
    freq = 1.0 / (ROTARY_BASE ** (jnp.arange(half_size, dtype=jnp.float32) / half_size))
    angle = positions[:, None] * freq[None, :]
    cosine = jnp.cos(angle)[:, None, :]
    sine = jnp.sin(angle)[:, None, :]
    front = block[..., :half_size]
    back = block[..., half_size:]
    return jnp.concatenate([front * cosine - back * sine, back * cosine + front * sine], axis=-1)


def pattern_attend(query, keys, values, lead_rows, dilation_step, low_row, high_row):
    rows_total, head_count, head_size = query.shape
    class_len = rows_total // dilation_step
    first_class = lead_rows // dilation_step - SIDE_SPAN
    class_q = query.reshape(class_len, dilation_step, head_count, head_size)
    class_k = keys.reshape(keys.shape[0] // dilation_step, dilation_step, head_count, head_size)
    class_v = values.reshape(values.shape[0] // dilation_step, dilation_step, head_count, head_size)
    sub_k = class_k[first_class:first_class + class_len + 2 * SIDE_SPAN]
    sub_v = class_v[first_class:first_class + class_len + 2 * SIDE_SPAN]
    if class_len <= SIDE_SPAN:
        block_len = class_len
        block_count = 1
        win_k = sub_k[None]
        win_v = sub_v[None]
        blocks_q = class_q[None]
    else:
        block_len = SIDE_SPAN
        block_count = class_len // SIDE_SPAN
        part_k = sub_k.reshape(block_count + 2, SIDE_SPAN, dilation_step, head_count, head_size)
        part_v = sub_v.reshape(block_count + 2, SIDE_SPAN, dilation_step, head_count, head_size)
        win_k = jnp.concatenate([part_k[:-2], part_k[1:-1], part_k[2:]], axis=1)
        win_v = jnp.concatenate([part_v[:-2], part_v[1:-1], part_v[2:]], axis=1)
        blocks_q = class_q.reshape(block_count, SIDE_SPAN, dilation_step, head_count, head_size)
    width = block_len + 2 * SIDE_SPAN
    scores = jnp.einsum('nasht,nksht->nshak', blocks_q, win_k, preferred_element_type=jnp.float32)
    scores = scores * (head_size ** -0.5)
    q_index = jnp.arange(block_len, dtype=jnp.int32)
    k_index = jnp.arange(width, dtype=jnp.int32)
    b_index = jnp.arange(block_count, dtype=jnp.int32)
    s_index = jnp.arange(dilation_step, dtype=jnp.int32)
    in_band = jnp.abs(k_index[None, :] - SIDE_SPAN - q_index[:, None]) <= SIDE_SPAN
    key_position = ((first_class + b_index[:, None] * block_len + k_index[None, :]) * dilation_step)[:, None, :] + s_index[None, :, None]
    is_valid = (key_position >= low_row) & (key_position < high_row)
    keep_mask = in_band[None, None, None] & is_valid[:, :, None, None, :]
    scores = jnp.where(keep_mask, scores, NEGATIVE)
    maxima = jnp.max(scores, axis=-1, keepdims=True)
    expo = jnp.exp(scores - maxima)
    totals = jnp.sum(expo, axis=-1)
    numerator = jnp.einsum('nshak,nksht->nasht', expo.astype(jnp.bfloat16), win_v, preferred_element_type=jnp.float32)
    totals_t = jnp.transpose(totals, (0, 3, 1, 2))
    result = (numerator / totals_t[..., None]).astype(jnp.bfloat16).reshape(rows_total, head_count, head_size)
    log_sum = jnp.transpose(maxima[..., 0] + jnp.log(totals), (0, 3, 1, 2)).reshape(rows_total, head_count)
    return result, log_sum


def combine(results):
    sums = jnp.stack([item[1] for item in results], axis=0)
    peak = jnp.max(sums, axis=0)
    share = jnp.exp(sums - peak[None])
    weight_sum = share[0] + share[1] + share[2]
    accum = share[0][..., None] * results[0][0].astype(jnp.float32)
    accum = accum + share[1][..., None] * results[1][0].astype(jnp.float32)
    accum = accum + share[2][..., None] * results[2][0].astype(jnp.float32)
    attended = (accum / weight_sum[..., None]).astype(jnp.bfloat16)
    return attended, peak + jnp.log(weight_sum)


def reference(tokens_in, w_query, w_key, w_value, w_out):
    positions = jnp.arange(TOKENS, dtype=jnp.float32)
    shape3 = (TOKENS, HEADS, HEAD_DIM)
    query = rotate(jnp.dot(tokens_in, w_query, preferred_element_type=jnp.float32).reshape(shape3), positions).astype(jnp.bfloat16)
    key = rotate(jnp.dot(tokens_in, w_key, preferred_element_type=jnp.float32).reshape(shape3), positions).astype(jnp.bfloat16)
    value = jnp.dot(tokens_in, w_value, preferred_element_type=jnp.float32).astype(jnp.bfloat16).reshape(shape3)
    query_h = jnp.transpose(query, (1, 0, 2))[:, :, None, :]
    key_h = jnp.transpose(key, (1, 0, 2))[:, :, None, :]
    value_h = jnp.transpose(value, (1, 0, 2))[:, :, None, :]

    def one_head(items):
        head_q, head_k, head_v = items
        results = []
        for dilation_step in (1, MIDDLE_DILATION, WIDEST_DILATION):
            border_extent = SIDE_SPAN * dilation_step
            pad_k = jnp.pad(head_k, ((border_extent, border_extent), (0, 0), (0, 0)))
            pad_v = jnp.pad(head_v, ((border_extent, border_extent), (0, 0), (0, 0)))
            results.append(pattern_attend(head_q, pad_k, pad_v, border_extent, dilation_step, border_extent, border_extent + TOKENS))
        attended, log_sum = combine(results)
        return attended[:, 0, :], log_sum[:, 0]

    attended_h, log_weight = lax.map(one_head, (query_h, key_h, value_h))
    attended = jnp.transpose(attended_h, (1, 0, 2)).reshape(TOKENS, HEADS * HEAD_DIM)
    group_cols = HEADS * HEAD_DIM // N_TP
    total = jnp.zeros((TOKENS, D), jnp.float32)
    for group in range(N_TP):
        part = jnp.dot(attended[:, group * group_cols:(group + 1) * group_cols],
                       w_out[group * group_cols:(group + 1) * group_cols], preferred_element_type=jnp.float32)
        rounded = lax.optimization_barrier(part.astype(jnp.bfloat16))
        total = total + rounded.astype(jnp.float32)
    return total.astype(jnp.bfloat16), log_weight
```

```python
import functools

import jax
import jax.numpy as jnp
import numpy as np
from jax import lax
from jax.experimental import pallas as pl
from jax.experimental.pallas import tpu as pltpu
from jax.sharding import PartitionSpec as P

HEAD_DIM = 64
SIDE_SPAN = 64
MIDDLE_DILATION = 8
WIDEST_DILATION = 64


ROTARY_BASE = 500000.0
NEGATIVE = -1e30


def shifted(block, axis, distance):
    devices = range(lax.axis_size(axis))
    route = [(i - distance, i) for i in devices if i - distance in devices]
    return lax.ppermute(block, axis, route)


def rotate(block, positions):
    half_size = block.shape[-1] // 2
    freq = 1.0 / ROTARY_BASE ** (jnp.arange(half_size, dtype=jnp.float32) / half_size)
    angle = positions[:, None] * freq[None, :]
    cosine = jnp.cos(angle)[:, None, :]
    sine = jnp.sin(angle)[:, None, :]
    front = block[..., :half_size]
    back = block[..., half_size:]
    return jnp.concatenate([front * cosine - back * sine, back * cosine + front * sine], axis=-1)


def pattern_attend(query, keys, values, lead_rows, dilation_step, low_row, high_row):
    rows_total, head_count, head_size = query.shape
    class_len = rows_total // dilation_step
    first_class = lead_rows // dilation_step - SIDE_SPAN
    class_q = query.reshape(class_len, dilation_step, head_count, head_size)
    class_k = keys.reshape(keys.shape[0] // dilation_step, dilation_step, head_count, head_size)
    class_v = values.reshape(values.shape[0] // dilation_step, dilation_step, head_count, head_size)
    sub_k = class_k[first_class : first_class + class_len + 2 * SIDE_SPAN]
    sub_v = class_v[first_class : first_class + class_len + 2 * SIDE_SPAN]
    if class_len <= SIDE_SPAN:
        block_len = class_len
        block_count = 1
        win_k = sub_k[None]
        win_v = sub_v[None]
        blocks_q = class_q[None]
    else:
        block_len = SIDE_SPAN
        block_count = class_len // SIDE_SPAN
        part_k = sub_k.reshape(block_count + 2, SIDE_SPAN, dilation_step, head_count, head_size)
        part_v = sub_v.reshape(block_count + 2, SIDE_SPAN, dilation_step, head_count, head_size)
        win_k = jnp.concatenate([part_k[:-2], part_k[1:-1], part_k[2:]], axis=1)
        win_v = jnp.concatenate([part_v[:-2], part_v[1:-1], part_v[2:]], axis=1)
        blocks_q = class_q.reshape(block_count, SIDE_SPAN, dilation_step, head_count, head_size)
    width = block_len + 2 * SIDE_SPAN
    scores = jnp.einsum("nasht,nksht->nshak", blocks_q, win_k, preferred_element_type=jnp.float32)
    scores = scores * head_size ** (-0.5)
    q_index = jnp.arange(block_len, dtype=jnp.int32)
    k_index = jnp.arange(width, dtype=jnp.int32)
    b_index = jnp.arange(block_count, dtype=jnp.int32)
    s_index = jnp.arange(dilation_step, dtype=jnp.int32)
    in_band = jnp.abs(k_index[None, :] - SIDE_SPAN - q_index[:, None]) <= SIDE_SPAN
    key_position = (
        (first_class + b_index[:, None] * block_len + k_index[None, :]) * dilation_step
    )[:, None, :] + s_index[None, :, None]
    is_valid = (key_position >= low_row) & (key_position < high_row)
    keep_mask = in_band[None, None, None] & is_valid[:, :, None, None, :]
    scores = jnp.where(keep_mask, scores, NEGATIVE)
    maxima = jnp.max(scores, axis=-1, keepdims=True)
    expo = jnp.exp(scores - maxima)
    totals = jnp.sum(expo, axis=-1)
    numerator = jnp.einsum(
        "nshak,nksht->nasht", expo.astype(jnp.bfloat16), win_v, preferred_element_type=jnp.float32
    )
    totals_t = jnp.transpose(totals, (0, 3, 1, 2))
    result = (
        (numerator / totals_t[..., None])
        .astype(jnp.bfloat16)
        .reshape(rows_total, head_count, head_size)
    )
    log_sum = jnp.transpose(maxima[..., 0] + jnp.log(totals), (0, 3, 1, 2)).reshape(
        rows_total, head_count
    )
    return (result, log_sum)


def combine(results):
    sums = jnp.stack([item[1] for item in results], axis=0)
    peak = jnp.max(sums, axis=0)
    share = jnp.exp(sums - peak[None])
    weight_sum = share[0] + share[1] + share[2]
    accum = share[0][..., None] * results[0][0].astype(jnp.float32)
    accum = accum + share[1][..., None] * results[1][0].astype(jnp.float32)
    accum = accum + share[2][..., None] * results[2][0].astype(jnp.float32)
    attended = (accum / weight_sum[..., None]).astype(jnp.bfloat16)
    return (attended, peak + jnp.log(weight_sum))


def per_device(tokens_in, w_query, w_key, w_value, w_out):
    col_count = w_query.shape[1]
    head_count = col_count // HEAD_DIM
    piece = lax.all_gather(tokens_in, "tp", axis=0, tiled=True)
    projected = jnp.concatenate(
        [
            jnp.dot(piece, w_query, preferred_element_type=jnp.float32),
            jnp.dot(piece, w_key, preferred_element_type=jnp.float32),
            jnp.dot(piece, w_value, preferred_element_type=jnp.float32),
        ],
        axis=1,
    )
    rows_total = projected.shape[0]
    sp_size = lax.axis_size("sp")
    sp_place = lax.axis_index("sp")
    positions = (sp_place * rows_total + jnp.arange(rows_total, dtype=jnp.int32)).astype(
        jnp.float32
    )
    shape3 = (rows_total, head_count, HEAD_DIM)
    query = rotate(projected[:, :col_count].reshape(shape3), positions).astype(jnp.bfloat16)
    keys = rotate(projected[:, col_count : 2 * col_count].reshape(shape3), positions).astype(
        jnp.bfloat16
    )
    values = projected[:, 2 * col_count :].astype(jnp.bfloat16).reshape(shape3)
    per_device_span = -(-(SIDE_SPAN * MIDDLE_DILATION) // rows_total)
    earlier_k = []
    earlier_v = []
    before_k, before_v = shifted((keys, values), "sp", 1)
    after_k, after_v = shifted((keys, values), "sp", -1)
    earlier_k.insert(0, before_k)
    earlier_v.insert(0, before_v)
    later_k = [after_k]
    later_v = [after_v]
    key_buf = jnp.concatenate(earlier_k + [keys] + later_k, axis=0)
    value_buf = jnp.concatenate(earlier_v + [values] + later_v, axis=0)
    lead_rows = per_device_span * rows_total
    low_row = lead_rows - sp_place * rows_total
    key_buf, value_buf, lead_rows, low_row, high_row = (
        key_buf,
        value_buf,
        lead_rows,
        low_row,
        low_row + sp_size * rows_total,
    )
    results = [
        pattern_attend(query, key_buf, value_buf, lead_rows, dilation_step, low_row, high_row)
        for dilation_step in (1, MIDDLE_DILATION)
    ]
    class_stride = WIDEST_DILATION // sp_size
    border_extent = SIDE_SPAN * class_stride
    class_shape = (rows_total // sp_size, sp_size, head_count, HEAD_DIM)
    parts = (
        lax.all_to_all(query.reshape(class_shape), "sp", split_axis=1, concat_axis=0, tiled=True),
        lax.all_to_all(keys.reshape(class_shape), "sp", split_axis=1, concat_axis=0, tiled=True),
        lax.all_to_all(values.reshape(class_shape), "sp", split_axis=1, concat_axis=0, tiled=True),
    )
    item_heads = parts[0].shape[2]
    flat = [item.reshape(rows_total, item_heads, HEAD_DIM) for item in parts]
    pad_k = jnp.pad(flat[1], ((border_extent, border_extent), (0, 0), (0, 0)))
    pad_v = jnp.pad(flat[2], ((border_extent, border_extent), (0, 0), (0, 0)))
    result, log_sum = pattern_attend(
        flat[0],
        pad_k,
        pad_v,
        border_extent,
        class_stride,
        border_extent,
        border_extent + rows_total,
    )
    result_back = lax.all_to_all(
        result.reshape(rows_total, 1, item_heads, HEAD_DIM),
        "sp",
        split_axis=0,
        concat_axis=1,
        tiled=True,
    )
    sum_back = lax.all_to_all(
        log_sum.reshape(rows_total, 1, item_heads), "sp", split_axis=0, concat_axis=1, tiled=True
    )
    results.append((result_back.reshape(shape3), sum_back.reshape(rows_total, head_count)))
    attended, log_weight = combine(results)
    flat_out = attended.reshape(rows_total, col_count)
    mixed = lax.psum_scatter(
        jnp.dot(flat_out, w_out, preferred_element_type=jnp.float32).astype(jnp.bfloat16),
        "tp",
        scatter_dimension=0,
        tiled=True,
    )
    return (mixed, jnp.transpose(log_weight, (1, 0)))


MESH_ID = pl.DeviceIdType.MESH
PAIR = 2 * HEAD_DIM
ROW_BLOCK = 128
SPLITS = 2
OUT_SPLITS = 4


def class_kernel(
    sp_size, tp_size, col_count,
    x_hbm, wq_hbm, wk_hbm, wv_hbm, wo_hbm, base_ref, local_cos, local_sin,
    out_ref, logw_ref,
    x_all, w_all, wo, cos_t, sin_t, q_c, kv_ext, pf, cls_send, cls_recv,
    bias_near, bias_class, o_near, lse_near, cls_o, cls_lse, ret, ret_lse, ret_f, lse_f, att,
    part_out, part_in, cross_out, cross_in, keep_b, keep_d,
    load_sem, own_send, own_recv, far_send, far_recv, fwd_send, fwd_recv,
    a2a_send, a2a_recv, halo_send, halo_recv, back_send, back_recv, lback_send, lback_recv,
    ex_send, ex_recv, cr_send, cr_recv,
):
    sp = lax.axis_index("sp")
    tp = lax.axis_index("tp")
    chips = tp_size // 2
    chip = tp // 2
    core = tp % 2
    partner = chip * 2 + (1 - core)
    shard = x_hbm.shape[0]
    rows = shard * tp_size
    piece = shard // SPLITS
    group_count = col_count // PAIR
    head_count = col_count // HEAD_DIM
    cls_rows = rows // sp_size
    chip_rows = 2 * shard
    chip_cls = chip_rows // sp_size
    f32, bf16 = jnp.float32, jnp.bfloat16

    def chip_at(d):
        return (chip + d) % chips

    loads = [pltpu.make_async_copy(x_hbm, x_all.at[tp], load_sem.at[0])]
    for n, w in enumerate((wq_hbm, wk_hbm, wv_hbm)):
        loads.append(pltpu.make_async_copy(w, w_all.at[n], load_sem.at[1 + n]))
    loads.append(pltpu.make_async_copy(wo_hbm, wo, load_sem.at[4]))
    for item in loads[:4]:
        item.start()

    barrier = pltpu.get_barrier_semaphore()
    pl.semaphore_signal(barrier, inc=1, device_id={"tp": partner}, device_id_type=MESH_ID)
    for d in range(1, chips):
        pl.semaphore_signal(
            barrier, inc=1, device_id={"tp": chip_at(d) * 2 + core}, device_id_type=MESH_ID
        )
    for off in range(1, sp_size):
        pl.semaphore_signal(
            barrier, inc=1, device_id={"sp": (sp + off) % sp_size}, device_id_type=MESH_ID
        )
    pl.semaphore_wait(barrier, 1 + (chips - 1) + (sp_size - 1))

    def remote(src, dst, send, recv, **where):
        return pltpu.make_async_remote_copy(
            src_ref=src, dst_ref=dst, send_sem=send, recv_sem=recv,
            device_id=where, device_id_type=MESH_ID,
        )

    waits = []
    far = {}
    for k in range(SPLITS):
        for d in range(1, chips):
            span = pl.ds(k * piece, piece)
            far[d, k] = remote(
                x_hbm.at[span], x_all.at[tp, span], far_send.at[d, k], far_recv.at[d, k],
                tp=chip_at(d) * 2 + core,
            )
            far[d, k].start()
            waits.append(far[d, k])
    own = remote(x_hbm, x_all.at[tp], own_send.at[0], own_recv.at[0], tp=partner)
    own.start()
    waits.append(own)
    loads[4].start()

    base_cos = base_ref[0, pl.ds(sp, 1), :]
    base_sin = base_ref[1, pl.ds(sp, 1), :]
    lane = lax.broadcasted_iota(jnp.int32, (1, PAIR), 1)
    front = lane % HEAD_DIM < HEAD_DIM // 2
    first_head = lane < HEAD_DIM
    sign = jnp.where(front, -1.0, 1.0).astype(f32)
    for r0 in range(0, rows, ROW_BLOCK):
        lc = local_cos[r0 : r0 + ROW_BLOCK]
        ls = local_sin[r0 : r0 + ROW_BLOCK]
        cos_t[r0 : r0 + ROW_BLOCK] = lc * base_cos - ls * base_sin
        sin_t[r0 : r0 + ROW_BLOCK] = (ls * base_cos + lc * base_sin) * sign
    window = ROW_BLOCK + 2 * SIDE_SPAN
    near_i = lax.broadcasted_iota(jnp.int32, (ROW_BLOCK, window), 0)
    near_j = lax.broadcasted_iota(jnp.int32, (ROW_BLOCK, window), 1)
    near_band = jnp.abs(near_j - SIDE_SPAN - near_i) <= SIDE_SPAN
    mid_step = MIDDLE_DILATION // sp_size
    wide_step = WIDEST_DILATION // sp_size
    for r0 in range(0, rows, ROW_BLOCK):
        key_pos = sp * rows + r0 + near_j - SIDE_SPAN
        good = near_band & (key_pos >= 0) & (key_pos < sp_size * rows)
        bias_near[r0 : r0 + ROW_BLOCK] = jnp.where(good, 0.0, NEGATIVE)
        gap = jnp.abs(
            lax.broadcasted_iota(jnp.int32, (ROW_BLOCK, rows), 0)
            + r0
            - lax.broadcasted_iota(jnp.int32, (ROW_BLOCK, rows), 1)
        )
        mid = (gap % mid_step == 0) & (gap <= SIDE_SPAN * mid_step)
        wide = (gap % wide_step == 0) & (gap <= SIDE_SPAN * wide_step)
        bias_class[r0 : r0 + ROW_BLOCK] = jnp.where(
            mid & wide, float(np.log(2.0)), jnp.where(mid | wide, 0.0, NEGATIVE)
        )

    def turn(x, cos, sin):
        swapped = jnp.where(
            front, pltpu.roll(x, PAIR - HEAD_DIM // 2, 1), pltpu.roll(x, HEAD_DIM // 2, 1)
        )
        return x * cos + swapped * sin

    def project(spans):
        for n in range(3):
            if len(spans) == 1:
                left = x_all[spans[0][0], pl.ds(spans[0][1], spans[0][2])]
            else:
                left = jnp.concatenate([x_all[s, pl.ds(a, c)] for s, a, c in spans], axis=0)
            full = jnp.dot(left, w_all[n], preferred_element_type=f32)
            at = 0
            for s, a, c in spans:
                r0 = pl.multiple_of(s * shard + a, c)
                cos = cos_t[pl.ds(r0, c)]
                sin = sin_t[pl.ds(r0, c)]
                for g in range(group_count):
                    part = full[at : at + c, g * PAIR : (g + 1) * PAIR]
                    if n < 2:
                        part = turn(part, cos, sin)
                    pf[n * group_count + g, pl.ds(r0, c), :] = part
                    low = part.astype(bf16)
                    if n == 0:
                        q_c[pl.ds(r0, c), g * PAIR : (g + 1) * PAIR] = low
                    else:
                        kv_ext[
                            pl.ds(r0 + SIDE_SPAN, c),
                            (n - 1) * col_count + g * PAIR : (n - 1) * col_count + (g + 1) * PAIR,
                        ] = low
                at += c

    a2a = {}

    def scatter(d):
        which = chip_at(d)
        base = pl.multiple_of(which * chip_cls, chip_cls)

        def one(r, carry):
            for g in range(3 * group_count):
                cls_send[r, pl.ds(base, chip_cls), g * PAIR : (g + 1) * PAIR] = pf[
                    g, pl.ds(which * chip_rows + r, chip_cls, stride=sp_size), :
                ].astype(bf16)
            return carry

        lax.fori_loop(0, sp_size, one, 0)
        mine = pl.ds(pl.multiple_of(sp * cls_rows + base, chip_cls), chip_cls)
        for off in range(1, sp_size):
            dest = (sp + off) % sp_size
            a2a[d, off] = remote(
                cls_send.at[dest, pl.ds(base, chip_cls)], cls_recv.at[mine],
                a2a_send.at[d, off], a2a_recv.at[d, off], sp=dest,
            )
            a2a[d, off].start()
        cls_recv[mine, :] = cls_send[sp, pl.ds(base, chip_cls), :]

    for item in loads[:4]:
        item.wait()
    project([(tp, 0, shard)])
    own.wait_recv()
    project([(partner, 0, shard)])
    scatter(0)
    fwd = {}
    for d in range(1, chips):
        src = chip_at(d) * 2 + core
        other = chip_at(d) * 2 + 1 - core
        e = chips - d
        for k in range(SPLITS):
            span = pl.ds(k * piece, piece)
            far[e, k].wait_recv()
            fwd[d, k] = remote(
                x_all.at[src, span], x_all.at[src, span], fwd_send.at[d, k], fwd_recv.at[d, k],
                tp=partner,
            )
            fwd[d, k].start()
            waits.append(fwd[d, k])
            fwd[d, k].wait_recv()
            project([(src, k * piece, piece), (other, k * piece, piece)])
        if d == chips - 1:
            halo = [
                remote(
                    kv_ext.at[pl.ds(rows, SIDE_SPAN)], kv_ext.at[pl.ds(0, SIDE_SPAN)],
                    halo_send.at[0], halo_recv.at[0], sp=(sp + 1) % sp_size,
                ),
                remote(
                    kv_ext.at[pl.ds(SIDE_SPAN, SIDE_SPAN)],
                    kv_ext.at[pl.ds(rows + SIDE_SPAN, SIDE_SPAN)],
                    halo_send.at[1], halo_recv.at[1], sp=(sp + sp_size - 1) % sp_size,
                ),
            ]
            for item in halo:
                item.start()
        scatter(d)

    lane_wide = lax.broadcasted_iota(jnp.int32, (ROW_BLOCK, PAIR), 1)
    scale = HEAD_DIM ** (-0.5)

    def attend(query, keys, values, bias):
        outs, sums = [], []
        for half in range(2):
            pick = first_head if half == 0 else jnp.logical_not(first_head)
            q = jnp.where(pick, query.astype(f32) * scale, 0.0).astype(bf16)
            s = lax.dot_general(q, keys, (((1,), (1,)), ((), ())), preferred_element_type=f32)
            s = s + bias
            top = jnp.max(s, axis=1, keepdims=True)
            e = jnp.exp(s - top)
            total = jnp.sum(e, axis=1, keepdims=True)
            o = jnp.dot(e.astype(bf16), values, preferred_element_type=f32)
            outs.append(o / total)
            sums.append(top + jnp.log(total))
        return jnp.where(first_head, outs[0], outs[1]), sums

    for item in halo:
        item.wait_recv()

    def near_pair(g, carry):
        c0 = pl.multiple_of(g * PAIR, PAIR)
        for r0 in range(0, rows, ROW_BLOCK):
            span = slice(r0, r0 + ROW_BLOCK)
            o, sums = attend(
                q_c[span, pl.ds(c0, PAIR)],
                kv_ext[r0 : r0 + window, pl.ds(c0, PAIR)],
                kv_ext[r0 : r0 + window, pl.ds(c0 + col_count, PAIR)],
                bias_near[span],
            )
            o_near[g, span, :] = o
            kept = lse_near[span]
            kept = jnp.where(lane_wide == 2 * g, sums[0], kept)
            lse_near[span] = jnp.where(lane_wide == 2 * g + 1, sums[1], kept)
        return carry

    lse_near[...] = jnp.zeros_like(lse_near)
    cls_lse[...] = jnp.zeros_like(cls_lse)
    lax.fori_loop(0, group_count, near_pair, 0)

    for d in range(chips):
        for off in range(1, sp_size):
            a2a[d, off].wait_recv()

    my_rows = pl.ds(pl.multiple_of(sp * cls_rows, cls_rows), cls_rows)

    def back(g, off):
        dest = (sp + off) % sp_size
        lanes = pl.ds(pl.multiple_of(g * PAIR, PAIR), PAIR)
        return remote(
            cls_o.at[pl.ds(pl.multiple_of(dest * cls_rows, cls_rows), cls_rows), lanes],
            ret.at[my_rows, lanes], back_send.at[g, off], back_recv.at[g, off], sp=dest,
        )

    def class_pair(g, carry):
        c0 = pl.multiple_of(g * PAIR, PAIR)
        keys = cls_recv[:, pl.ds(c0 + col_count, PAIR)]
        values = cls_recv[:, pl.ds(c0 + 2 * col_count, PAIR)]
        for r0 in range(0, rows, ROW_BLOCK):
            span = slice(r0, r0 + ROW_BLOCK)
            o, sums = attend(cls_recv[span, pl.ds(c0, PAIR)], keys, values, bias_class[span])
            cls_o[span, pl.ds(c0, PAIR)] = o.astype(bf16)
            kept = cls_lse[span]
            kept = jnp.where(lane_wide == 2 * g, sums[0], kept)
            cls_lse[span] = jnp.where(lane_wide == 2 * g + 1, sums[1], kept)
        for off in range(1, sp_size):
            back(g, off).start()
        ret[my_rows, pl.ds(c0, PAIR)] = cls_o[my_rows, pl.ds(c0, PAIR)]
        return carry

    lax.fori_loop(0, group_count, class_pair, 0)
    lback = []
    for off in range(1, sp_size):
        dest = (sp + off) % sp_size
        item = remote(
            cls_lse.at[pl.ds(pl.multiple_of(dest * cls_rows, cls_rows), cls_rows)],
            ret_lse.at[my_rows], lback_send.at[off], lback_recv.at[off], sp=dest,
        )
        item.start()
        lback.append(item)
    ret_lse[my_rows, :] = cls_lse[my_rows, :]
    loads[4].wait()
    for item in lback:
        item.wait_recv()
    for r in range(sp_size):
        lse_f[pl.ds(r, cls_rows, stride=sp_size), :] = ret_lse[r * cls_rows : (r + 1) * cls_rows]
    for g in range(group_count):
        for off in range(1, sp_size):
            back(g, off).wait_recv()
        for r in range(sp_size):
            ret_f[g, pl.ds(r, cls_rows, stride=sp_size), :] = ret[
                r * cls_rows : (r + 1) * cls_rows, g * PAIR : (g + 1) * PAIR
            ].astype(f32)

    for r0 in range(0, rows, ROW_BLOCK):
        span = slice(r0, r0 + ROW_BLOCK)
        la = lse_near[span]
        lb = lse_f[span]
        peak = jnp.maximum(la, lb)
        ea = jnp.exp(la - peak)
        eb = jnp.exp(lb - peak)
        total = ea + eb
        logw = peak + jnp.log(total)
        logw_ref[:, span] = jnp.transpose(logw)[:head_count]
        ea = ea / total
        eb = eb / total
        for g in range(group_count):
            wa = jnp.where(first_head, ea[:, 2 * g : 2 * g + 1], ea[:, 2 * g + 1 : 2 * g + 2])
            wb = jnp.where(first_head, eb[:, 2 * g : 2 * g + 1], eb[:, 2 * g + 1 : 2 * g + 2])
            mixed = wa * o_near[g, span, :] + wb * ret_f[g, span, :]
            att[span, g * PAIR : (g + 1) * PAIR] = mixed.astype(bf16)

    width = wo.shape[1] // OUT_SPLITS

    def product(place, n):
        left = att[pl.ds(pl.multiple_of(place * shard, shard), shard), :]
        return jnp.dot(left, wo[:, n * width : (n + 1) * width], preferred_element_type=f32).astype(bf16)

    exch, cross = {}, {}
    steps = [(d, n) for d in range(1, chips) for n in range(OUT_SPLITS)]

    def relay(d, n):
        exch[d, n].wait_recv()
        cross_out[d, n] = (keep_b[d, n].astype(f32) + part_in[d, n].astype(f32)).astype(bf16)
        cross[d, n] = remote(
            cross_out.at[d, n], cross_in.at[d, n], cr_send.at[d, n], cr_recv.at[d, n],
            tp=chip_at(d) * 2 + core,
        )
        cross[d, n].start()
        waits.append(cross[d, n])

    def exchange(d, n):
        part_out[d, n] = product(chip_at(d) * 2 + 1 - core, n)
        exch[d, n] = remote(
            part_out.at[d, n], part_in.at[d, n], ex_send.at[d, n], ex_recv.at[d, n], tp=partner
        )
        exch[d, n].start()
        waits.append(exch[d, n])

    for at, (d, n) in enumerate(steps):
        exchange(d, n)
        keep_b[d, n] = product(chip_at(d) * 2 + core, n)
        if at:
            relay(*steps[at - 1])
    relay(*steps[-1])
    for n in range(OUT_SPLITS):
        exchange(0, n)
        keep_d[n] = product(tp, n)
    for n in range(OUT_SPLITS):
        exch[0, n].wait_recv()
        total = keep_d[n].astype(f32) + part_in[0, n].astype(f32)
        for d in range(1, chips):
            cross[d, n].wait_recv()
            total = total + cross_in[d, n].astype(f32)
        out_ref[:, n * width : (n + 1) * width] = total.astype(bf16)

    for item in waits:
        item.wait_send()
    for item in a2a.values():
        item.wait_send()
    for item in halo:
        item.wait_send()
    for item in lback:
        item.wait_send()
    for g in range(group_count):
        for off in range(1, sp_size):
            back(g, off).wait_send()


def fused(sp_size, tp_size, tokens_in, w_query, w_key, w_value, w_out):
    shard, depth = tokens_in.shape
    col_count = w_query.shape[1]
    rows = shard * tp_size
    chips = tp_size // 2
    groups = col_count // PAIR
    cls_rows = rows // sp_size
    wide = w_out.shape[1]
    width = wide // OUT_SPLITS
    half = HEAD_DIM // 2
    freq = 1.0 / ROTARY_BASE ** (np.arange(half) / half)
    freq = np.tile(freq, PAIR // half)
    local = np.arange(rows)[:, None] * freq[None, :]
    start = (np.arange(sp_size) * rows)[:, None] * freq[None, :]
    base = jnp.asarray(np.stack([np.cos(start), np.sin(start)]).astype(np.float32))
    local_cos = jnp.asarray(np.cos(local).astype(np.float32))
    local_sin = jnp.asarray(np.sin(local).astype(np.float32))
    f32, bf16 = jnp.float32, jnp.bfloat16
    V, DMA = pltpu.VMEM, pltpu.SemaphoreType.DMA
    window = ROW_BLOCK + 2 * SIDE_SPAN
    scratch = [
        V((tp_size, shard, depth), bf16),
        V((3, depth, col_count), bf16),
        V((col_count, wide), bf16),
        V((rows, PAIR), f32),
        V((rows, PAIR), f32),
        V((rows, col_count), bf16),
        V((rows + 2 * SIDE_SPAN, 2 * col_count), bf16),
        V((3 * groups, rows, PAIR), f32),
        V((sp_size, cls_rows, 3 * col_count), bf16),
        V((rows, 3 * col_count), bf16),
        V((rows, window), f32),
        V((rows, rows), f32),
        V((groups, rows, PAIR), f32),
        V((rows, PAIR), f32),
        V((rows, col_count), bf16),
        V((rows, PAIR), f32),
        V((rows, col_count), bf16),
        V((rows, PAIR), f32),
        V((groups, rows, PAIR), f32),
        V((rows, PAIR), f32),
        V((rows, col_count), bf16),
        V((chips, OUT_SPLITS, shard, width), bf16),
        V((chips, OUT_SPLITS, shard, width), bf16),
        V((chips, OUT_SPLITS, shard, width), bf16),
        V((chips, OUT_SPLITS, shard, width), bf16),
        V((chips, OUT_SPLITS, shard, width), bf16),
        V((OUT_SPLITS, shard, width), bf16),
        DMA((5,)),
        DMA((1,)), DMA((1,)),
        DMA((chips, SPLITS)), DMA((chips, SPLITS)),
        DMA((chips, SPLITS)), DMA((chips, SPLITS)),
        DMA((chips, sp_size)), DMA((chips, sp_size)),
        DMA((2,)), DMA((2,)),
        DMA((groups, sp_size)), DMA((groups, sp_size)),
        DMA((sp_size,)), DMA((sp_size,)),
        DMA((chips, OUT_SPLITS)), DMA((chips, OUT_SPLITS)),
        DMA((chips, OUT_SPLITS)), DMA((chips, OUT_SPLITS)),
    ]
    any_spec = pl.BlockSpec(memory_space=pl.ANY)
    vmem = pl.BlockSpec(memory_space=pltpu.VMEM)
    return pl.pallas_call(
        functools.partial(class_kernel, sp_size, tp_size, col_count),
        out_shape=(
            jax.ShapeDtypeStruct((shard, wide), bf16),
            jax.ShapeDtypeStruct((col_count // HEAD_DIM, rows), f32),
        ),
        in_specs=[any_spec] * 5 + [vmem] * 3,
        out_specs=(vmem, vmem),
        scratch_shapes=scratch,
        compiler_params=pltpu.CompilerParams(
            collective_id=0, has_side_effects=True, vmem_limit_bytes=66 * 1024 * 1000
        ),
        name="dilated_layer",
    )(tokens_in, w_query, w_key, w_value, w_out, base, local_cos, local_sin)


def solution(mesh):
    in_specs = (P(("sp", "tp"), None), P(None, "tp"), P(None, "tp"), P(None, "tp"), P("tp", None))
    out_specs = (P(("sp", "tp"), None), P("tp", "sp"))
    sp_size, tp_size = mesh.shape["sp"], mesh.shape["tp"]

    def body(*args):
        rows = args[0].shape[0] * tp_size
        whole_class = (
            MIDDLE_DILATION % sp_size == 0
            and rows % (sp_size * ROW_BLOCK // 4) == 0
            and tp_size % 2 == 0
            and tp_size > 2
        )
        if whole_class:
            return fused(sp_size, tp_size, *args)
        return per_device(*args)

    return jax.shard_map(body, mesh=mesh, in_specs=in_specs, out_specs=out_specs, check_vma=False)
```
